32 devices in a mesh: ep: 8 (over z, x), tp: 4 (over y, core).
Axes of the slice: x: 2, y: 2, z: 4, core: 2. Of those that a mesh axis runs over, the one named last changes fastest.
Arguments:
- queries: bfloat16 [1024, 2048], P('ep', 'tp'), may hold values from -60 to 60
- keys: bfloat16 [1024, 512], P('ep', 'tp'), may hold values from -60 to 60
- values: bfloat16 [1024, 512], P('ep', 'tp'), may hold values from -6 to 6
- cum_gates: float32 [1024, 16], P('ep', 'tp'), may hold values from -259 to 0, as said below
- expert_in: bfloat16 [4096, 4096], P(('ep', 'tp')), may hold values from -6 to 6
- norm_gain: float32 [4096], replicated, may hold values from 0.1 to 1.9
- route_group: int32 [4096, 1], P(('ep', 'tp')), may hold values from 0 to 7; in each aligned block of 128 rows (0 to 127, 128 to 255, ...) at most 24 rows name the same one
- route_member: int32 [4096, 2], P(('ep', 'tp')), may hold values from 0 to 3, all different within a row
- route_weight: float32 [4096, 2], P(('ep', 'tp')), may hold values from 0.1 to 1
- w_gate: bfloat16 [32, 4096, 384], P(('ep', 'tp')), may hold values from -0.09375 to 0.09375
- w_up: bfloat16 [32, 4096, 384], P(('ep', 'tp')), may hold values from -0.09375 to 0.09375
- w_down: bfloat16 [32, 384, 4096], P(('ep', 'tp')), may hold values from -0.3125 to 0.3125
Outputs:
- attended: bfloat16 [1024, 2048], P('ep', 'tp')
- expert_out: bfloat16 [4096, 4096], P(('ep', 'tp'))
The draws below stay inside these ranges and needn't reach their ends.
Inputs may be any that keep to these rules, and one draw needn't show every extreme that they name: `cum_gates`: each head's entries never rise along positions. `route_group`: at most 24 of the rows of one device name one group. `route_member`: the 2 entries of a row differ.
All inputs are finite; a program needn't handle non-finite values.
Results may differ from the reference program's by a relative error of at most 0.0075.
Values may be sent and summed in bfloat16 or wider, within the bound.
No kernel may reach another device: no remote copies, remote signals or barrier semaphores. Data moves between devices by JAX's collectives and lax.ppermute only.
A program may use at most 128 MiB of HBM per device.

```python
import math
import jax
import jax.numpy as jnp
import numpy as np
from jax import lax

D = 4096
HEAD_WIDTH = 128
QUERY_HEADS = 16
KEY_VALUE_HEADS = 4
FF = 384
GROUP = 4
TOP = 2
TOK_A = 128
TOK_B = 128
ATTENDED_LENGTH = 1024
TOKENS_B = 4096
CAP = 24
EXPERTS = 32
N_EP = 8
N_TP = 4


def draw_keys(key, part):
    base_value = jax.random.normal(jax.random.fold_in(key, 1), (ATTENDED_LENGTH, KEY_VALUE_HEADS, HEAD_WIDTH), jnp.float32)
    return base_value.reshape(ATTENDED_LENGTH, KEY_VALUE_HEADS * HEAD_WIDTH).astype(jnp.bfloat16)


def draw_queries(key, part):
    heads_per_group = QUERY_HEADS // KEY_VALUE_HEADS
    base_value = jax.random.normal(jax.random.fold_in(key, 2), (ATTENDED_LENGTH, KEY_VALUE_HEADS, heads_per_group, HEAD_WIDTH), jnp.float32)
    return base_value.reshape(ATTENDED_LENGTH, QUERY_HEADS * HEAD_WIDTH).astype(jnp.bfloat16)


def draw_cum_gates(key, part):
    share = 0.5
    slow_heads = jax.random.uniform(jax.random.fold_in(key, 3), (QUERY_HEADS,), jnp.float32) < share
    slow_rate = jnp.exp(jax.random.uniform(jax.random.fold_in(key, 4), (QUERY_HEADS,), jnp.float32, math.log(0.3), 0.0)) / ATTENDED_LENGTH
    fast_rate = 1.0 / jnp.exp(jax.random.uniform(jax.random.fold_in(key, 5), (QUERY_HEADS,), jnp.float32, math.log(30.0), math.log(100.0)))
    rates = jnp.where(slow_heads, slow_rate, fast_rate)
    block_count = ATTENDED_LENGTH // TOK_A
    block_factor = jnp.exp(jax.random.uniform(jax.random.fold_in(key, 6), (block_count,), jnp.float32, math.log(0.5), math.log(2.0)))
    position_factor = jnp.repeat(block_factor, TOK_A)
    roughness = jax.random.uniform(jax.random.fold_in(key, 7), (ATTENDED_LENGTH, QUERY_HEADS), jnp.float32, 0.2, 1.8)
    gate_logarithms = -rates[None, :] * position_factor[:, None] * roughness
    spike_positions = jax.random.randint(jax.random.fold_in(key, 8), (3,), 1, ATTENDED_LENGTH)
    spike_loss = jax.random.uniform(jax.random.fold_in(key, 9), (3, QUERY_HEADS), jnp.float32, 0.2, 0.5)
    spike_values = jnp.zeros((ATTENDED_LENGTH, QUERY_HEADS), jnp.float32).at[spike_positions].add(jnp.log1p(-spike_loss))
    return jnp.cumsum(gate_logarithms + spike_values, axis=0)


def shard_levels(stream_key, dims, pieces, least, largest):
    factor_of, own = 1.0, jax.random.fold_in(stream_key, 6)
    for dim, shards_of in pieces:
        draws = jnp.exp(jax.random.uniform(jax.random.fold_in(own, dim), (shards_of,), jnp.float32, least / len(pieces), largest / len(pieces)))
        factor_of = factor_of * jnp.repeat(draws, dims[dim] // shards_of).reshape([-1 if axis == dim else 1 for axis in range(len(dims))])
    return factor_of


def choose_distinct(key, rows, count, top, lift):
    order = jax.random.permutation(jax.random.fold_in(key, 1), count)
    boost = order
    for power in range(3):
        boost = boost * boost // count
    boost = boost * lift // count
    chance = jax.random.randint(jax.random.fold_in(key, 2), (rows, count), 0, 4096) + boost
    sure = jax.random.permutation(jax.random.fold_in(key, 3), rows)[jnp.arange(count) % rows]
    chance = jnp.where(jnp.arange(rows)[:, None] == sure[None, :], 1 << 14, chance)
    priority = chance * count + jnp.arange(count)
    return lax.top_k(priority.astype(jnp.int32), top)[1].astype(jnp.int32)


def routed_block(own_key, own, number, rows, number_of, top, most, slope):
    sequence = jax.random.permutation(own_key, number_of)
    packed, ordinary = portions_of(number_of, rows * top, most, slope, True), portions_of(number_of, rows * top, most, slope, False)
    places = jnp.arange(number_of)

    def named(sizes, turn):
        used = int((sizes > 0).sum())
        fixed = max(1, used // 4)
        moved = fixed + (places - fixed + turn * (used - fixed)) % max(1, number_of - fixed)
        return jnp.zeros((number_of,), jnp.int32).at[sequence[jnp.where(places < fixed, places, moved)]].set(jnp.asarray(sizes, jnp.int32))

    sizes = jnp.where(number % 4 == 0, named(packed, number // 4), named(ordinary, number - number // 4 - 1))
    mixed = jax.random.permutation(jax.random.fold_in(own, 3), number_of)
    source_of, taker = mixed[0:number_of // 2 * 2:2], mixed[1:number_of // 2 * 2:2]
    margin = jnp.minimum(sizes[source_of] - 1, most - sizes[taker]) // 2
    margin = jnp.where((source_of == sequence[0]) | (taker == sequence[0]) | (sizes[taker] == 0), 0, jnp.maximum(margin, 0))
    moved = jax.random.randint(jax.random.fold_in(own, 4), (number_of // 2,), 0, 1 << 20) % (margin + 1)
    sizes = sizes.at[source_of].add(-moved).at[taker].add(moved)
    items = jnp.searchsorted(jnp.cumsum(sizes), jnp.arange(rows * top), side="right").astype(jnp.int32)
    grid = items.reshape(top, rows).T
    grid = grid[jax.random.permutation(jax.random.fold_in(own, 1), rows)]
    turn = jax.random.randint(jax.random.fold_in(own, 2), (rows, 1), 0, top)
    return jnp.take_along_axis(grid, (jnp.arange(top)[None, :] + turn) % top, axis=1)


def portions_of(count, total, reach, slope, full):
    portions = [(1 << 20) // math.isqrt(rank ** slope) + 1 for rank in range(1, count + 1)]
    largest = reach if full else min(reach, max(-(-total // count), total * portions[0] // sum(portions)))
    least = 1 if total - largest >= count - 1 else 0
    holding, spare = [largest] + [least] * (count - 1), total - largest - least * (count - 1)
    while spare > 0:
        candidates = [i for i in range(1, count) if holding[i] < largest] or [i for i in range(1, count) if holding[i] < reach]
        pool, left = sum([portions[i] for i in candidates]), spare
        for i in candidates:
            extra = min(reach - holding[i], max(1, left * portions[i] // pool), spare)
            holding[i] = holding[i] + extra
            spare = spare - extra
    return np.array(holding)


def scatter_about(own_key, shape, scale, bound, cuts=(), held_as=jnp.bfloat16):
    level = shard_levels(own_key, shape, cuts, -0.22, 0.18) if cuts else 1.0
    drawn = jax.random.normal(own_key, shape, jnp.float32) * scale * level
    return jnp.minimum(jnp.maximum(drawn, -bound), bound).astype(held_as)


def setup_inputs(seed: int = 0) -> dict:
    seeds = jax.random.split(jax.random.key(seed), 13)
    queries = draw_queries(jax.random.fold_in(seeds[12], 71), 0)
    keys = draw_keys(jax.random.fold_in(seeds[12], 71), 0)
    values = scatter_about(seeds[2], (ATTENDED_LENGTH, KEY_VALUE_HEADS * HEAD_WIDTH), 1.0, 6.0, ((0, 8), (1, 4)))
    cum_gates = draw_cum_gates(jax.random.fold_in(seeds[12], 71), 0)
    expert_in = scatter_about(seeds[4], (TOKENS_B, D), 1.0, 6.0, ((0, 32),))
    norm_gain = jnp.clip(1.0 + 0.18 * jax.random.normal(seeds[5], (D,), jnp.float32), 0.1, 1.9)
    route_group_keys = jax.random.split(jax.random.fold_in(seeds[6], 1), TOKENS_B // TOK_B)
    route_group_turns = jax.random.permutation(jax.random.fold_in(seeds[6], 3), TOKENS_B // TOK_B)
    route_group = jax.vmap(lambda own, number: routed_block(jax.random.fold_in(seeds[6], 2), own, number, TOK_B, N_EP, 1, CAP, 2))(route_group_keys, route_group_turns).reshape((TOKENS_B, 1))
    route_member = choose_distinct(seeds[7], TOKENS_B, GROUP, TOP, 0)
    route_weight = jnp.clip(jnp.exp(math.log(1.0) - 2.3025851 * jax.random.uniform(seeds[8], (TOKENS_B, TOP), jnp.float32) ** shard_levels(seeds[8], (TOKENS_B, TOP), ((0, 32),), -0.2, 0.2)), 0.1, 1.0)
    w_gate = scatter_about(seeds[9], (EXPERTS, D, FF), D ** -0.5, 0.09375, ((0, 32),))
    w_up = scatter_about(seeds[10], (EXPERTS, D, FF), D ** -0.5, 0.09375, ((0, 32),))
    w_down = scatter_about(seeds[11], (EXPERTS, FF, D), FF ** -0.5, 0.3125, ((0, 32),))
    return {"queries": queries, "keys": keys, "values": values, "cum_gates": cum_gates, "expert_in": expert_in, "norm_gain": norm_gain, "route_group": route_group, "route_member": route_member, "route_weight": route_weight, "w_gate": w_gate, "w_up": w_up, "w_down": w_down}


NEGATIVE = -1e+30
EPSILON = 1e-06

def attention_part(queries, keys, values, cum_gates):
    sequence_length = queries.shape[0]
    heads_per_group = QUERY_HEADS // KEY_VALUE_HEADS
    rows_per_block = math.gcd(sequence_length, 512)
    score_scale = HEAD_WIDTH ** (-0.5)
    every_query = queries.reshape(sequence_length, KEY_VALUE_HEADS, heads_per_group, HEAD_WIDTH).astype(jnp.float32)
    every_key = keys.reshape(sequence_length, KEY_VALUE_HEADS, HEAD_WIDTH).astype(jnp.float32)
    every_value = values.reshape(sequence_length, KEY_VALUE_HEADS, HEAD_WIDTH).astype(jnp.float32)

    def query_block(block_index):
        start_row = block_index * rows_per_block
        query_rows = lax.dynamic_slice_in_dim(every_query, start_row, rows_per_block, 0)
        query_gates = lax.dynamic_slice_in_dim(cum_gates, start_row, rows_per_block, 0)
        query_pos = start_row + jnp.arange(rows_per_block, dtype=jnp.int32)

        def key_step(key_index, carried):
            running, totals, accumulated = carried
            key_start = (key_index * rows_per_block).astype(jnp.int32)
            key_rows = lax.dynamic_slice_in_dim(every_key, key_start, rows_per_block, 0)
            rows_of_value = lax.dynamic_slice_in_dim(every_value, key_start, rows_per_block, 0)
            key_gates = lax.dynamic_slice_in_dim(cum_gates, key_start, rows_per_block, 0)
            key_pos = key_start + jnp.arange(rows_per_block, dtype=jnp.int32)
            scores = jnp.einsum('qgrd,kgd->grqk', query_rows, key_rows).reshape(QUERY_HEADS, rows_per_block, rows_per_block) * score_scale
            scores = scores + query_gates.T[:, :, None] - key_gates.T[:, None, :]
            allowed = (key_pos[None, :] <= query_pos[:, None])[None]
            scores = jnp.where(allowed, scores, NEGATIVE)
            new_max = jnp.maximum(running, lax.optimization_barrier(jnp.max(scores, axis=-1)))
            weights = jnp.where(allowed, jnp.exp(scores - new_max[..., None]), 0.0)
            factor = jnp.exp(running - new_max)
            totals = totals * factor + lax.optimization_barrier(jnp.sum(weights, axis=-1))
            rounded_count = lax.optimization_barrier(weights.astype(jnp.bfloat16)).astype(jnp.float32)
            inner_product = jnp.einsum('tjub,btl->tjul', rounded_count.reshape(KEY_VALUE_HEADS, heads_per_group, rows_per_block, rows_per_block), rows_of_value)
            accumulated = accumulated * factor[..., None] + inner_product.reshape(QUERY_HEADS, rows_per_block, HEAD_WIDTH)
            return (new_max, totals, accumulated)
        initial = (jnp.full((QUERY_HEADS, rows_per_block), NEGATIVE, jnp.float32), jnp.zeros((QUERY_HEADS, rows_per_block), jnp.float32), jnp.zeros((QUERY_HEADS, rows_per_block, HEAD_WIDTH), jnp.float32))
        running, totals, accumulated = lax.fori_loop(0, block_index + 1, key_step, initial)
        result = accumulated / totals[..., None]
        return jnp.transpose(result, (1, 0, 2)).reshape(rows_per_block, QUERY_HEADS * HEAD_WIDTH).astype(jnp.bfloat16)
    blocks = lax.map(query_block, jnp.arange(sequence_length // rows_per_block, dtype=jnp.int32))
    return blocks.reshape(sequence_length, QUERY_HEADS * HEAD_WIDTH)

def expert_part(expert_in, norm_gain, route_group, route_member, route_weight, w_gate, w_up, w_down):
    count_rows, model_width = expert_in.shape
    floats = expert_in.astype(jnp.float32)
    normed = (floats * lax.rsqrt(lax.optimization_barrier(jnp.mean(floats * floats, axis=-1, keepdims=True)) + EPSILON) * norm_gain).astype(jnp.bfloat16)
    members = jnp.arange(GROUP, dtype=jnp.int32)
    mix_weights = jnp.zeros((count_rows, GROUP), jnp.float32)
    for rank_index in range(TOP):
        mix_weights = mix_weights + route_weight[:, rank_index:rank_index + 1] * (route_member[:, rank_index:rank_index + 1] == members[None, :]).astype(jnp.float32)
    mix_weights = lax.optimization_barrier(mix_weights.astype(jnp.bfloat16)).astype(jnp.float32)
    group_ids = route_group[:, 0]
    group_match = (group_ids[:, None] == jnp.arange(N_EP, dtype=jnp.int32)[None, :]).astype(jnp.int32)
    rank_within = lax.optimization_barrier(jnp.sum((jnp.cumsum(group_match, axis=0) - group_match) * group_match, axis=1)).astype(jnp.int32)
    slots_per_group = CAP * N_EP * N_TP
    row_table = jnp.full((N_EP, slots_per_group), count_rows, jnp.int32).at[group_ids, rank_within].set(jnp.arange(count_rows, dtype=jnp.int32))
    padded_rows = jnp.concatenate([normed, jnp.zeros((1, model_width), jnp.bfloat16)], axis=0)
    padded_weights = jnp.concatenate([mix_weights, jnp.zeros((1, GROUP), jnp.float32)], axis=0)

    def one_group(group_index):
        row_index = row_table[group_index]
        rows_in = padded_rows[row_index]
        weights_in = padded_weights[row_index]
        combined = jnp.zeros((slots_per_group, model_width), jnp.float32)
        for member in range(GROUP):
            expert_index = group_index * GROUP + member
            gate_part = jnp.dot(rows_in, w_gate[expert_index], preferred_element_type=jnp.float32)
            up_part = jnp.dot(rows_in, w_up[expert_index], preferred_element_type=jnp.float32)
            hidden = (jax.nn.silu(gate_part) * up_part).astype(jnp.bfloat16)
            outputs = jnp.dot(hidden, w_down[expert_index], preferred_element_type=jnp.float32).astype(jnp.bfloat16)
            combined = combined + weights_in[:, member:member + 1] * outputs.astype(jnp.float32)
        return combined.astype(jnp.bfloat16)
    results = lax.map(one_group, jnp.arange(N_EP, dtype=jnp.int32))
    table_out = jnp.zeros((count_rows + 1, model_width), jnp.bfloat16).at[row_table.reshape(-1)].set(results.reshape(-1, model_width))
    return table_out[:count_rows]

def reference(queries, keys, values, cum_gates, expert_in, norm_gain, route_group, route_member, route_weight, w_gate, w_up, w_down):
    attended = attention_part(queries, keys, values, cum_gates)
    expert_out = expert_part(expert_in, norm_gain, route_group, route_member, route_weight, w_gate, w_up, w_down)
    return (attended, expert_out)
```

```python
import functools
import math

import jax
import jax.numpy as jnp
from jax import lax
from jax.experimental import pallas as pl
from jax.experimental.pallas import tpu as pltpu
from jax.sharding import PartitionSpec as P

HEAD_WIDTH = 128
GROUP = 4
TOP = 2
LANES = 128


NEGATIVE = -1e30
EPSILON = 1e-06


def group_fold(states, prepared_group, key_piece, value_piece, start_row, all_gates, key_heads):
    query_rows, query_pos, query_gates = prepared_group
    count_queries = query_rows.shape[0]
    head_count = all_gates.shape[1]
    heads_per_group = head_count // key_heads
    piece_rows = key_piece.shape[0]
    rows_per_block = math.gcd(piece_rows, 512)
    score_scale = HEAD_WIDTH ** (-0.5)

    def key_step(step_index, carried):
        running, totals, accumulated = carried
        offset = step_index * rows_per_block
        key_rows = lax.dynamic_slice_in_dim(key_piece, offset, rows_per_block, 0).reshape(
            rows_per_block, key_heads, HEAD_WIDTH
        )
        rows_of_value = lax.dynamic_slice_in_dim(value_piece, offset, rows_per_block, 0).reshape(
            rows_per_block, key_heads, HEAD_WIDTH
        )
        key_gates = lax.dynamic_slice_in_dim(all_gates, offset, rows_per_block, 0)
        key_pos = offset + jnp.arange(rows_per_block, dtype=jnp.int32)
        scores = jnp.einsum(
            "qgrd,kgd->grqk", query_rows, key_rows, preferred_element_type=jnp.float32
        )
        scores = scores.reshape(head_count, count_queries, rows_per_block) * score_scale
        scores = scores + query_gates.T[:, :, None] - key_gates.T[:, None, :]
        allowed = (key_pos[None, :] <= query_pos[:, None])[None]
        scores = jnp.where(allowed, scores, NEGATIVE)
        new_max = jnp.maximum(running, jnp.max(scores, axis=-1))
        weights = jnp.where(allowed, jnp.exp(scores - new_max[..., None]), 0.0)
        factor = jnp.exp(running - new_max)
        totals = totals * factor + jnp.sum(weights, axis=-1)
        inner_product = jnp.einsum(
            "tjub,btl->tjul",
            weights.astype(jnp.bfloat16).reshape(
                key_heads, heads_per_group, count_queries, rows_per_block
            ),
            rows_of_value,
            preferred_element_type=jnp.float32,
        )
        accumulated = accumulated * factor[..., None] + inner_product.reshape(
            head_count, count_queries, HEAD_WIDTH
        )
        return (new_max, totals, accumulated)

    def run_all(carried):
        return lax.fori_loop(0, piece_rows // rows_per_block, key_step, carried)

    def keep_state(carried):
        return carried

    return lax.cond(start_row <= query_pos[-1], run_all, keep_state, states)


def fold_attention(groups, keys, values, all_gates):
    key_heads = keys.shape[1] // HEAD_WIDTH
    head_count = all_gates.shape[1]
    prepared = []
    initial = []
    for query_block, query_pos in groups:
        count_queries = query_block.shape[0]
        prepared.append(
            (
                query_block.reshape(count_queries, key_heads, head_count // key_heads, HEAD_WIDTH),
                query_pos,
                all_gates[query_pos],
            )
        )
        initial.append(
            (
                jnp.full((head_count, count_queries), NEGATIVE, jnp.float32),
                jnp.zeros((head_count, count_queries), jnp.float32),
                jnp.zeros((head_count, count_queries, HEAD_WIDTH), jnp.float32),
            )
        )
    carried = tuple(initial)
    start_row = jnp.int32(0)
    key_piece = lax.all_gather(keys, "ep", axis=0, tiled=True)
    value_piece = lax.all_gather(values, "ep", axis=0, tiled=True)
    finals = tuple(
        (
            group_fold(
                states, prepared_group, key_piece, value_piece, start_row, all_gates, key_heads
            )
            for states, prepared_group in zip(carried, prepared)
        )
    )
    outputs = []
    for running, totals, accumulated in finals:
        result = accumulated / totals[..., None]
        outputs.append(
            jnp.transpose(result, (1, 0, 2))
            .reshape(result.shape[1], head_count * HEAD_WIDTH)
            .astype(jnp.bfloat16)
        )
    return outputs


def attention_half(queries, keys, values, cum_gates):
    count_rows = queries.shape[0]
    head_count = cum_gates.shape[1]
    ep_index = lax.axis_index("ep")
    all_gates = lax.all_gather(cum_gates, "ep", axis=0, tiled=True)
    query_heads = queries.reshape(count_rows, head_count, HEAD_WIDTH)
    positions = ep_index * count_rows + jnp.arange(count_rows, dtype=jnp.int32)
    outputs = fold_attention([(query_heads, positions)], keys, values, all_gates)
    attended = outputs[0]
    return attended


def expert_half(
    expert_in, norm_gain, route_group, route_member, route_weight, w_gate, w_up, w_down
):
    count_rows, model_width = expert_in.shape
    ep_size = lax.axis_size("ep")
    tp_size = lax.axis_size("tp")
    capacity = max(2, (3 * count_rows + 2 * ep_size - 1) // (2 * ep_size))
    floats = expert_in.astype(jnp.float32)
    normed = (
        floats * lax.rsqrt(jnp.mean(floats * floats, axis=-1, keepdims=True) + EPSILON) * norm_gain
    ).astype(jnp.bfloat16)
    members = jnp.arange(GROUP, dtype=jnp.int32)
    mix_weights = jnp.zeros((count_rows, GROUP), jnp.float32)
    for rank_index in range(TOP):
        mix_weights = mix_weights + route_weight[:, rank_index : rank_index + 1] * (
            route_member[:, rank_index : rank_index + 1] == members[None, :]
        ).astype(jnp.float32)
    mix_weights = mix_weights.astype(jnp.bfloat16)
    group_ids = route_group[:, 0]
    group_match = (group_ids[:, None] == jnp.arange(ep_size, dtype=jnp.int32)[None, :]).astype(
        jnp.int32
    )
    rank_within = jnp.sum((jnp.cumsum(group_match, axis=0) - group_match) * group_match, axis=1)
    slot_of_row = group_ids * capacity + rank_within
    row_of_slot = (
        jnp.full((ep_size * capacity,), count_rows, jnp.int32)
        .at[slot_of_row]
        .set(jnp.arange(count_rows, dtype=jnp.int32))
    )
    padded_rows = jnp.concatenate([normed, jnp.zeros((1, model_width), jnp.bfloat16)], axis=0)
    padded_weights = jnp.concatenate([mix_weights, jnp.zeros((1, GROUP), jnp.bfloat16)], axis=0)
    send_rows = padded_rows[row_of_slot].reshape(ep_size, capacity, model_width)
    send_weights = padded_weights[row_of_slot].reshape(ep_size, capacity, GROUP)
    gate_matrix = w_gate[0]
    up_matrix = w_up[0]
    down_matrix = w_down[0]
    arrived_rows = lax.all_to_all(send_rows, "ep", split_axis=0, concat_axis=0, tiled=True)
    arrived_weights = lax.all_to_all(send_weights, "ep", split_axis=0, concat_axis=0, tiled=True)
    sources = arrived_rows.shape[0]
    per_source = arrived_rows.shape[1]
    flat_rows = arrived_rows.reshape(sources * per_source, model_width)
    pieces = lax.all_gather(flat_rows, "tp", axis=0, tiled=True)
    gate_part = jnp.dot(pieces, gate_matrix, preferred_element_type=jnp.float32)
    up_part = jnp.dot(pieces, up_matrix, preferred_element_type=jnp.float32)
    hidden = (jax.nn.silu(gate_part) * up_part).astype(jnp.bfloat16)
    expert_outputs = jnp.dot(hidden, down_matrix, preferred_element_type=jnp.float32).astype(
        jnp.bfloat16
    )
    member_outputs = lax.all_to_all(
        expert_outputs.reshape(tp_size, sources * per_source, model_width),
        "tp",
        split_axis=0,
        concat_axis=0,
        tiled=True,
    )
    flat_weights = arrived_weights.reshape(sources * per_source, GROUP).astype(jnp.float32)
    combined = jnp.zeros((sources * per_source, model_width), jnp.float32)
    for member in range(GROUP):
        combined = combined + flat_weights[:, member : member + 1] * member_outputs[member]
    mixed = combined.astype(jnp.bfloat16).reshape(sources, per_source, model_width)
    returned = lax.all_to_all(mixed, "ep", split_axis=0, concat_axis=0, tiled=True)
    return returned.reshape(ep_size * capacity, model_width)[slot_of_row]


def general_device(
    queries,
    keys,
    values,
    cum_gates,
    expert_in,
    norm_gain,
    route_group,
    route_member,
    route_weight,
    w_gate,
    w_up,
    w_down,
):
    attended = attention_half(queries, keys, values, cum_gates)
    expert_out = expert_half(
        expert_in, norm_gain, route_group, route_member, route_weight, w_gate, w_up, w_down
    )
    return (attended, expert_out)


def pack_kernel(
    slots, me_ref, x_ref, gain_ref, group_ref, member_ref, weight_ref, key_ref, value_ref, gates_ref,
    *refs,
):
    pieces, pick_ref, pack_ref, normed_ref = refs[:-3], refs[-3], refs[-2], refs[-1]
    ep_size = len(pieces)
    count_rows, model_width = x_ref.shape
    step = min(16, count_rows)

    def norm_rows(index, carried):
        rows = pl.ds(pl.multiple_of(index * step, step), step)
        floats = x_ref[rows, :].astype(jnp.float32)
        scale = lax.rsqrt(jnp.mean(floats * floats, axis=-1, keepdims=True) + EPSILON)
        normed_ref[rows, :] = (floats * scale * gain_ref[...]).astype(jnp.bfloat16)
        return carried

    lax.fori_loop(0, count_rows // step, norm_rows, 0)
    relative = jnp.bitwise_xor(group_ref[...], me_ref[0])
    match = (
        relative == lax.broadcasted_iota(jnp.int32, (ep_size, count_rows), 0)
    ).astype(jnp.float32)
    earlier = (
        lax.broadcasted_iota(jnp.int32, (count_rows, count_rows), 0)
        < lax.broadcasted_iota(jnp.int32, (count_rows, count_rows), 1)
    ).astype(jnp.bfloat16)
    ranks = jnp.dot(match.astype(jnp.bfloat16), earlier, preferred_element_type=jnp.float32)
    rank = jnp.sum(ranks * match, axis=0, keepdims=True).astype(jnp.int32)
    slot = relative * slots + rank
    total = ep_size * slots
    pick = (slot == lax.broadcasted_iota(jnp.int32, (total, count_rows), 0)).astype(jnp.float32)
    pick_ref[...] = jnp.transpose(pick).astype(jnp.bfloat16)
    pick = pick.astype(jnp.bfloat16)
    members = lax.broadcasted_iota(jnp.int32, (LANES, count_rows), 0)
    mix = jnp.zeros((LANES, count_rows), jnp.float32)
    for k in range(member_ref.shape[0]):
        mix = mix + jnp.where(member_ref[k : k + 1, :] == members, weight_ref[k : k + 1, :], 0.0)
    mixed = lax.dot_general(
        pick, mix.astype(jnp.bfloat16), (((1,), (1,)), ((), ())), preferred_element_type=jnp.float32
    ).astype(jnp.bfloat16)
    for index, piece in enumerate(pieces):
        piece[:, model_width:] = mixed[index * slots : (index + 1) * slots]
    width = min(512, model_width)
    for start in range(0, model_width, width):
        columns = slice(start, start + width)
        rows = jnp.dot(pick, normed_ref[:, columns], preferred_element_type=jnp.float32)
        for index, piece in enumerate(pieces):
            piece[:, columns] = rows[index * slots : (index + 1) * slots].astype(jnp.bfloat16)
    pack_ref[:count_rows, :HEAD_WIDTH] = key_ref[...]
    pack_ref[:count_rows, HEAD_WIDTH:] = value_ref[...]
    gates = gates_ref[...]
    high = gates.astype(jnp.bfloat16).astype(jnp.float32)
    middle = (gates - high).astype(jnp.bfloat16).astype(jnp.float32)
    low = gates - high - middle
    pack_ref[count_rows:, :HEAD_WIDTH] = jnp.concatenate([high, middle], axis=0).astype(jnp.bfloat16)
    pack_ref[count_rows:, HEAD_WIDTH:] = jnp.concatenate(
        [low, jnp.zeros_like(low)], axis=0
    ).astype(jnp.bfloat16)


def pack_call(me, expert_in, norm_gain, groups, members, weights, keys, values, gates, ep_size, slots):
    count_rows, model_width = expert_in.shape
    head_count = gates.shape[0]
    piece = jax.ShapeDtypeStruct((slots, model_width + LANES), jnp.bfloat16)
    vmem = pl.BlockSpec(memory_space=pltpu.VMEM)
    return pl.pallas_call(
        functools.partial(pack_kernel, slots),
        out_shape=[piece] * ep_size
        + [
            jax.ShapeDtypeStruct((count_rows, ep_size * slots), jnp.bfloat16),
            jax.ShapeDtypeStruct((count_rows + 2 * head_count, 2 * HEAD_WIDTH), jnp.bfloat16),
        ],
        in_specs=[pl.BlockSpec(memory_space=pltpu.SMEM)] + [vmem] * 8,
        out_specs=[vmem] * (ep_size + 2),
        scratch_shapes=[pltpu.VMEM((count_rows, model_width), jnp.bfloat16)],
        compiler_params=pltpu.CompilerParams(vmem_limit_bytes=16 << 20),
        name="pack",
    )(me, expert_in, norm_gain, groups, members, weights, keys, values, gates)


def expert_kernel(me_ref, a_ref, b_ref, c_ref, d_ref, gate_ref, up_ref, down_ref, pa_ref, pb_ref, ps_ref):
    rows_each = a_ref.shape[0]
    model_width = gate_ref.shape[0]
    member = me_ref[0]
    refs = (a_ref, b_ref, c_ref, d_ref)
    depth = min(1024, model_width)
    gate_part = up_part = None
    for start in range(0, model_width, depth):
        inner = slice(start, start + depth)
        rows = jnp.concatenate([ref[:, inner] for ref in refs], axis=0)
        one = jnp.dot(rows, gate_ref[inner, :], preferred_element_type=jnp.float32)
        two = jnp.dot(rows, up_ref[inner, :], preferred_element_type=jnp.float32)
        gate_part = one if gate_part is None else gate_part + one
        up_part = two if up_part is None else up_part + two
    hidden = ((gate_part / (1.0 + jnp.exp(-gate_part))) * up_part).astype(jnp.bfloat16)
    mixes = jnp.concatenate([ref[:, model_width:] for ref in refs], axis=0).astype(jnp.float32)
    chosen = lax.broadcasted_iota(jnp.int32, mixes.shape, 1) == member
    mix = jnp.sum(jnp.where(chosen, mixes, 0.0), axis=1, keepdims=True)
    width = min(1024, model_width)
    for start in range(0, model_width, width):
        columns = slice(start, start + width)
        out = jnp.dot(hidden, down_ref[:, columns], preferred_element_type=jnp.float32)
        out = (out.astype(jnp.bfloat16).astype(jnp.float32) * mix).astype(jnp.bfloat16)
        pa_ref[:, columns] = out[:rows_each]
        pb_ref[:, columns] = out[rows_each : 2 * rows_each]
        ps_ref[:, columns] = out[2 * rows_each :]


def expert_call(me, a, b, c, d, gate_matrix, up_matrix, down_matrix):
    rows_each = a.shape[0]
    model_width = gate_matrix.shape[0]
    vmem = pl.BlockSpec(memory_space=pltpu.VMEM)
    part = jax.ShapeDtypeStruct((rows_each, model_width), jnp.bfloat16)
    return pl.pallas_call(
        expert_kernel,
        out_shape=[part, part, jax.ShapeDtypeStruct((2 * rows_each, model_width), jnp.bfloat16)],
        in_specs=[pl.BlockSpec(memory_space=pltpu.SMEM)] + [vmem] * 7,
        out_specs=[vmem] * 3,
        compiler_params=pltpu.CompilerParams(vmem_limit_bytes=40 << 20),
        name="expert",
    )(me, a, b, c, d, gate_matrix, up_matrix, down_matrix)


def attention_kernel(me_ref, q_ref, gates_ref, *refs):
    packs, out_ref = refs[:-1], refs[-1]
    count_rows = q_ref.shape[0]
    head_count = gates_ref.shape[0]
    me = me_ref[0]
    scale = HEAD_WIDTH ** (-0.5)
    row = lax.broadcasted_iota(jnp.int32, (count_rows, count_rows), 0) + me * count_rows
    column = lax.broadcasted_iota(jnp.int32, (count_rows, count_rows), 1)
    blocks = []
    for step, pack in enumerate(packs):
        first = me - 2 * step
        for half in range(2):
            owner = first if half == 0 else jnp.bitwise_xor(first, 1)
            offset = jnp.where(first >= 0, owner, me + 1) * count_rows
            allowed = column + offset <= row
            tail = pack[half, count_rows:, :].astype(jnp.float32)
            gates = (
                tail[:head_count, :HEAD_WIDTH] + tail[head_count:, :HEAD_WIDTH]
            ) + tail[:head_count, HEAD_WIDTH:]
            blocks.append((pack, half, allowed, gates))
    own = jnp.concatenate([gates_ref[...], jnp.zeros_like(gates_ref[...])], axis=0)
    own = jnp.transpose(own)
    for head in range(head_count):
        lanes = slice(head * HEAD_WIDTH, (head + 1) * HEAD_WIDTH)
        q = q_ref[:, lanes]
        scores = []
        top = None
        for pack, half, allowed, gates in blocks:
            s = lax.dot_general(
                q,
                pack[half, :count_rows, :HEAD_WIDTH],
                (((1,), (1,)), ((), ())),
                preferred_element_type=jnp.float32,
            )
            s = s * scale + own[:, head : head + 1] - gates[head : head + 1, :]
            s = jnp.where(allowed, s, NEGATIVE)
            scores.append(s)
            top = s if top is None else jnp.maximum(top, s)
        top = jnp.max(top, axis=1, keepdims=True)
        total = None
        result = None
        for (pack, half, allowed, gates), s in zip(blocks, scores):
            w = jnp.where(allowed, jnp.exp(s - top), 0.0)
            total = w if total is None else total + w
            part = jnp.dot(
                w.astype(jnp.bfloat16),
                pack[half, :count_rows, HEAD_WIDTH:],
                preferred_element_type=jnp.float32,
            )
            result = part if result is None else result + part
        total = jnp.sum(total, axis=1, keepdims=True)
        out_ref[:, lanes] = (result / total).astype(jnp.bfloat16)


def attention_call(me, queries, gates, packs):
    vmem = pl.BlockSpec(memory_space=pltpu.VMEM)
    return pl.pallas_call(
        attention_kernel,
        out_shape=jax.ShapeDtypeStruct(queries.shape, jnp.bfloat16),
        in_specs=[pl.BlockSpec(memory_space=pltpu.SMEM)] + [vmem] * (2 + len(packs)),
        out_specs=vmem,
        compiler_params=pltpu.CompilerParams(vmem_limit_bytes=24 << 20),
        name="attend",
    )(me, queries, gates, *packs)


def return_kernel(pick_ref, *refs):
    pieces, out_ref = refs[:-1], refs[-1]
    model_width = out_ref.shape[1]
    width = min(512, model_width)
    for start in range(0, model_width, width):
        columns = slice(start, start + width)
        rows = jnp.concatenate([piece[:, columns] for piece in pieces], axis=0)
        out_ref[:, columns] = jnp.dot(
            pick_ref[...], rows, preferred_element_type=jnp.float32
        ).astype(jnp.bfloat16)


def return_call(pick, pieces):
    vmem = pl.BlockSpec(memory_space=pltpu.VMEM)
    return pl.pallas_call(
        return_kernel,
        out_shape=jax.ShapeDtypeStruct((pick.shape[0], pieces[0].shape[1]), jnp.bfloat16),
        in_specs=[vmem] * (1 + len(pieces)),
        out_specs=vmem,
        compiler_params=pltpu.CompilerParams(vmem_limit_bytes=16 << 20),
        name="place",
    )(pick, *pieces)


def swap(array, axis, distance):
    size = lax.axis_size(axis)
    return lax.ppermute(array, axis, [(i, i ^ distance) for i in range(size)])


def paired_device(
    queries,
    keys,
    values,
    cum_gates,
    expert_in,
    norm_gain,
    route_group,
    route_member,
    route_weight,
    w_gate,
    w_up,
    w_down,
):
    count_rows, model_width = expert_in.shape
    ep_size = lax.axis_size("ep")
    slots = max(2, (3 * count_rows + 2 * ep_size - 1) // (2 * ep_size))
    ep_index = lax.axis_index("ep").astype(jnp.int32).reshape(1)
    tp_index = lax.axis_index("tp").astype(jnp.int32).reshape(1)
    gates = cum_gates.T
    *pieces, pick, pack = pack_call(
        ep_index,
        expert_in,
        norm_gain.reshape(1, model_width),
        route_group.T,
        route_member.T,
        route_weight.T,
        keys,
        values,
        gates,
        ep_size,
        slots,
    )
    arrived = [pieces[0]] + [swap(pieces[d], "ep", d) for d in range(1, ep_size)]
    packs = [jnp.stack([pack, swap(pack, "ep", 1)])]
    for _ in range(ep_size // 2 - 1):
        packs.append(
            lax.ppermute(packs[-1], "ep", [(i, i + 2) for i in range(ep_size - 2)])
        )
    returned = [None] * ep_size
    for d in range(0, ep_size, 2):
        a = jnp.concatenate([arrived[d], arrived[d + 1]], axis=0)
        b = swap(a, "tp", 2)
        c = swap(a, "tp", 1)
        far = swap(b, "tp", 1)
        pa, pb, ps = expert_call(tp_index, a, b, c, far, w_gate[0], w_up[0], w_down[0])
        back = swap(ps, "tp", 1).astype(jnp.float32)
        rows = 2 * slots
        crossing = (pb.astype(jnp.float32) + back[rows:]).astype(jnp.bfloat16)
        crossed = swap(crossing, "tp", 2)
        mixed = (pa.astype(jnp.float32) + back[:rows] + crossed.astype(jnp.float32)).astype(
            jnp.bfloat16
        )
        for half in range(2):
            part = mixed[half * slots : (half + 1) * slots]
            returned[d + half] = part if d + half == 0 else swap(part, "ep", d + half)
    attended = attention_call(ep_index, queries, gates, packs)
    expert_out = return_call(pick, returned)
    return (attended, expert_out)


def solution(mesh):
    ep_size, tp_size = mesh.shape["ep"], mesh.shape["tp"]
    paired = tp_size == GROUP and ep_size <= 16 and ep_size & (ep_size - 1) == 0
    per_device = paired_device if paired else general_device

    return jax.shard_map(
        per_device,
        mesh=mesh,
        in_specs=(
            P("ep", "tp"),
            P("ep", "tp"),
            P("ep", "tp"),
            P("ep", "tp"),
            P(("ep", "tp"), None),
            P(),
            P(("ep", "tp"), None),
            P(("ep", "tp"), None),
            P(("ep", "tp"), None),
            P(("ep", "tp"), None, None),
            P(("ep", "tp"), None, None),
            P(("ep", "tp"), None, None),
        ),
        out_specs=(P("ep", "tp"), P(("ep", "tp"), None)),
        check_vma=False,
    )
```
